32 devices in a mesh: sp: 16 (over z, y, x), tp: 2 (over core).
Axes of the slice: x: 2, y: 2, z: 4, core: 2. Of those that a mesh axis runs over, the one named last changes fastest.
Arguments:
- stream: bfloat16 [7168, 2048], P('sp'), may hold values from -6 to 6
- norm_gain: float32 [2, 2048], replicated, may hold values from 0.1 to 1.9
- value_weight: bfloat16 [2, 2048, 512], P(None, None, 'tp'), may hold values from -0.125 to 0.125
- gate_weight: bfloat16 [2, 2048, 512], P(None, None, 'tp'), may hold values from -0.125 to 0.125
- conv_taps: bfloat16 [2, 512, 512], P(None, None, 'tp'), may hold values from -0.25 to 0.25
- conv_bias: float32 [2, 512], P(None, 'tp'), may hold values from -3 to 3
- channel_gain: float32 [2, 512], replicated, may hold values from 0.1 to 1.9
- channel_shift: float32 [2, 512], replicated, may hold values from -3 to 3
- out_weight: bfloat16 [2, 512, 2048], replicated, may hold values from -0.25 to 0.25
Outputs:
- result: bfloat16 [7168, 2048], P('sp')
The draws below stay inside these ranges and needn't reach their ends.
All inputs are finite; a program needn't handle non-finite values.
Results may differ from the reference program's by a relative error of at most 0.0075.
Values may be sent and summed in bfloat16 or wider, within the bound.
No kernel may reach another device: no remote copies, remote signals or barrier semaphores. Data moves between devices by JAX's collectives and lax.ppermute only.
A program may use at most 64 MiB of HBM per device.

```python
import jax
import jax.numpy as jnp
from jax import lax

D = 2048
CH = 512
KW = 512
LAYERS = 2
TOKENS = 7168


def block_scale(key, shape, pieces, smallest, high):
    loudness, own = 1.0, jax.random.fold_in(key, 6)
    for dim, parts in pieces:
        steps = jnp.exp(jax.random.uniform(jax.random.fold_in(own, dim), (parts,), jnp.float32, smallest / len(pieces), high / len(pieces)))
        loudness = loudness * jnp.repeat(steps, shape[dim] // parts).reshape([-1 if axis == dim else 1 for axis in range(len(shape))])
    return loudness


def scatter_about(stream_key, dims, scale, most, split=(), held_as=jnp.bfloat16):
    array = scale * jax.random.normal(stream_key, dims, jnp.float32)
    if split:
        array = array * block_scale(stream_key, dims, split, -0.22, 0.18)
    return jnp.clip(array, -most, most).astype(held_as)


def setup_inputs(seed: int = 0) -> dict:
    key_list = jax.random.split(jax.random.key(seed), 10)
    stream = scatter_about(key_list[0], (TOKENS, D), 1.0, 6.0, ((0, 16),))
    norm_gain = jnp.clip(1.0 + 0.18 * jax.random.normal(key_list[1], (LAYERS, D), jnp.float32), 0.1, 1.9)
    value_weight = scatter_about(key_list[2], (LAYERS, D, CH), D ** -0.5, 0.125, ((2, 2),))
    gate_weight = scatter_about(key_list[3], (LAYERS, D, CH), D ** -0.5, 0.125, ((2, 2),))
    conv_taps = scatter_about(key_list[4], (LAYERS, KW, CH), KW ** -0.5, 0.25, ((2, 2),))
    conv_bias = scatter_about(key_list[5], (LAYERS, CH), 0.5, 3.0, ((1, 2),), jnp.float32)
    channel_gain = jnp.clip(1.0 + 0.18 * jax.random.normal(key_list[6], (LAYERS, CH), jnp.float32), 0.1, 1.9)
    channel_shift = scatter_about(key_list[7], (LAYERS, CH), 0.5, 3.0, (), jnp.float32)
    out_weight = scatter_about(key_list[8], (LAYERS, CH, D), CH ** -0.5, 0.25)
    return dict(stream=stream, norm_gain=norm_gain, value_weight=value_weight, gate_weight=gate_weight, conv_taps=conv_taps, conv_bias=conv_bias, channel_gain=channel_gain, channel_shift=channel_shift, out_weight=out_weight)


def rms_normed(stream, gain):
    values = stream.astype(jnp.float32)
    scale = lax.rsqrt(lax.optimization_barrier(jnp.mean(values * values, axis=-1, keepdims=True)) + 1e-06)
    return (values * scale * gain[None, :]).astype(jnp.bfloat16)

def channel_mix(conv, gain, shift):
    values = conv.astype(jnp.float32)
    center = lax.optimization_barrier(jnp.mean(values, axis=-1, keepdims=True))
    spread = lax.optimization_barrier(jnp.mean(jnp.square(values - center), axis=-1, keepdims=True))
    normed = (values - center) * lax.rsqrt(spread + 1e-05) * gain[None, :] + shift[None, :]
    return jax.nn.silu(normed).astype(jnp.bfloat16)

def causal_conv(gated, taps):
    length = gated.shape[0]
    span = taps.shape[0]
    padded_len = 1 << (length + span - 2).bit_length()
    signal = jnp.fft.rfft(gated.astype(jnp.float32), n=padded_len, axis=0)
    kernel = jnp.fft.rfft(taps.astype(jnp.float32)[::-1], n=padded_len, axis=0)
    return jnp.fft.irfft(signal * kernel, n=padded_len, axis=0)[:length]

def reference(stream, norm_gain, value_weight, gate_weight, conv_taps, conv_bias, channel_gain, channel_shift, out_weight):
    state = stream
    for layer in range(LAYERS):
        normed = rms_normed(state, norm_gain[layer])
        values = jnp.dot(normed, value_weight[layer], preferred_element_type=jnp.float32)
        gates = jnp.dot(normed, gate_weight[layer], preferred_element_type=jnp.float32)
        gated = (values * jax.nn.sigmoid(gates)).astype(jnp.bfloat16)
        conv = causal_conv(gated, conv_taps[layer])
        conv = (conv + conv_bias[layer][None, :]).astype(jnp.bfloat16)
        mixed = channel_mix(conv, channel_gain[layer], channel_shift[layer])
        update = jnp.dot(mixed, out_weight[layer], preferred_element_type=jnp.float32)
        state = (state.astype(jnp.float32) + update).astype(jnp.bfloat16)
    return state
```

```python
import functools

import jax
import jax.numpy as jnp
import numpy as np
from jax import lax
from jax.experimental import pallas as pl
from jax.experimental.pallas import tpu as pltpu
from jax.sharding import PartitionSpec as P

STEP = 32


def passed_along(value, axis, by):
    count = lax.axis_size(axis)
    pairs = [(i, i + by) for i in range(count) if 0 <= i + by < count]
    return lax.ppermute(value, axis, pairs)


def rms_normed(stream, gain):
    values = stream.astype(jnp.float32)
    scale = lax.rsqrt(jnp.mean(values * values, axis=-1, keepdims=True) + 1e-06)
    return (values * scale * gain[None, :]).astype(jnp.bfloat16)


def channel_mix(conv, gain, shift):
    values = conv.astype(jnp.float32)
    center = jnp.mean(values, axis=-1, keepdims=True)
    spread = jnp.mean(jnp.square(values - center), axis=-1, keepdims=True)
    normed = (values - center) * lax.rsqrt(spread + 1e-05) * gain[None, :] + shift[None, :]
    return jax.nn.silu(normed).astype(jnp.bfloat16)


def gate_rows(normed, w_value, w_gate):
    values = jnp.dot(normed, w_value, preferred_element_type=jnp.float32)
    gates = jnp.dot(normed, w_gate, preferred_element_type=jnp.float32)
    return (values * jax.nn.sigmoid(gates)).astype(jnp.bfloat16)


def rotations(rows, cols, row_at, col_at, unit, scale):
    col = col_at(np.arange(cols, dtype=np.float64))
    coarse = row_at(np.arange(0, rows, STEP, dtype=np.float64))
    fine = row_at(np.arange(STEP, dtype=np.float64)) - row_at(np.float64(0))
    a = unit * np.outer(coarse, col)
    b = unit * np.outer(fine, col)
    both = [scale * np.cos(a), scale * np.sin(a), np.cos(b), np.sin(b)]
    return [x.astype(np.float32) for x in both]


def split(value, hi_ref, lo_ref, rows):
    hi = value.astype(jnp.bfloat16)
    hi_ref[rows, :] = hi
    lo_ref[rows, :] = (value - hi.astype(jnp.float32)).astype(jnp.bfloat16)


def spread_out(tables, outs):
    ca, sa, cb, sb = tables
    c_hi, c_lo, s_hi, s_lo = outs

    for i in range(ca.shape[0]):
        rows = pl.ds(i * STEP, STEP)
        c1 = ca[i : i + 1, :]
        s1 = sa[i : i + 1, :]
        c2 = cb[...]
        s2 = sb[...]
        split(c1 * c2 - s1 * s2, c_hi, c_lo, rows)
        split(s1 * c2 + c1 * s2, s_hi, s_lo, rows)


def dot(a, b):
    return jnp.dot(a, b, preferred_element_type=jnp.float32)


def prep_kernel(*refs):
    own_t, halo_t, back_t = refs[0:4], refs[4:8], refs[8:12]
    taps = refs[12]
    own, halo, back = refs[13:17], refs[17:21], refs[21:25]
    tap_c, tap_s = refs[25:27]
    spread_out(halo_t, halo)
    for layer in range(taps.shape[0]):
        t = taps[layer]
        tap_c[layer] = dot(halo[0][...], t) + dot(halo[1][...], t)
        tap_s[layer] = dot(halo[2][...], t) + dot(halo[3][...], t)
    spread_out(own_t, own)
    spread_out(back_t, back)


def own_kernel(c_hi, c_lo, s_hi, s_lo, gated, w_c, w_s):
    g = gated[...]
    w_c[...] = dot(c_hi[...], g) + dot(c_lo[...], g)
    w_s[...] = dot(s_hi[...], g) + dot(s_lo[...], g)


def parts(value):
    hi = value.astype(jnp.bfloat16)
    return hi, (value - hi.astype(jnp.float32)).astype(jnp.bfloat16)


def finish_kernel(*refs, layer, pieces):
    halo, back = refs[0:4], refs[4:8]
    tap_c, tap_s, own_c, own_s, bias = refs[8:13]
    got = refs[13 : 13 + pieces]
    out = refs[13 + pieces]
    window = jnp.concatenate([g[...] for g in got], axis=0)
    w_c = own_c[...] + dot(halo[0][...], window) + dot(halo[1][...], window)
    w_s = own_s[...] + dot(halo[2][...], window) + dot(halo[3][...], window)
    h_c = tap_c[layer]
    h_s = tap_s[layer]
    re_hi, re_lo = parts(w_c * h_c + w_s * h_s)
    im_hi, im_lo = parts(w_s * h_c - w_c * h_s)
    y = dot(back[0][...], re_hi) + dot(back[2][...], im_hi)
    y += dot(back[1][...], re_hi) + dot(back[3][...], im_hi)
    y += dot(back[0][...], re_lo) + dot(back[2][...], im_lo)
    out[...] = (y + bias[layer : layer + 1, :]).astype(jnp.bfloat16)


def cost(flops, size):
    return pl.CostEstimate(flops=flops, bytes_accessed=size, transcendentals=0)


def per_device(
    stream,
    norm_gain,
    value_weight,
    gate_weight,
    conv_taps,
    conv_bias,
    channel_gain,
    channel_shift,
    out_weight,
):
    tokens = stream.shape[0]
    layers, width, chans = conv_taps.shape
    halo_rows = -(-(width - 1) // 16) * 16
    hops = -(-halo_rows // tokens)
    size = -(-(tokens + halo_rows) // (2 * STEP)) * (2 * STEP)
    half = size // 2
    unit = 2 * np.pi / size
    bf16, f32 = jnp.bfloat16, jnp.float32
    assert tokens % STEP == 0 and halo_rows >= width

    def freq(k):
        return k + 0.5

    own_tab = rotations(half, tokens, freq, lambda t: t + 1, unit, 1.0)
    halo_tab = rotations(half, halo_rows, freq, lambda i: i + 1 - halo_rows, unit, 1.0)
    back_tab = rotations(tokens, half, lambda t: t + 1, freq, unit, 2.0 / size)
    taps = conv_taps
    if halo_rows > width:
        taps = jnp.pad(conv_taps, ((0, 0), (halo_rows - width, 0), (0, 0)))

    mats = [(half, tokens)] * 4 + [(half, halo_rows)] * 4 + [(tokens, half)] * 4
    shapes = [jax.ShapeDtypeStruct(m, bf16) for m in mats]
    shapes += [jax.ShapeDtypeStruct((layers, half, chans), f32)] * 2
    made = pl.pallas_call(
        prep_kernel,
        out_shape=shapes,
        cost_estimate=cost(4 * layers * size * halo_rows * chans, 8 << 20),
        name="prep",
    )(*own_tab, *halo_tab, *back_tab, taps)
    own_m, halo_m, back_m, tap_f = made[0:4], made[4:8], made[8:12], made[12:14]

    state = stream
    for layer in range(layers):
        normed = rms_normed(state, norm_gain[layer])
        own_gated = gate_rows(normed, value_weight[layer], gate_weight[layer])
        pieces = []
        for step in range(1, hops + 1):
            count = min(tokens, halo_rows - (step - 1) * tokens)
            pieces.insert(0, passed_along(own_gated[tokens - count :], "sp", step))
        own_f = pl.pallas_call(
            own_kernel,
            out_shape=[jax.ShapeDtypeStruct((half, chans), f32)] * 2,
            cost_estimate=cost(4 * size * tokens * chans, 4 << 20),
            name="own_part",
        )(*own_m, own_gated)
        conv = pl.pallas_call(
            functools.partial(finish_kernel, layer=layer, pieces=len(pieces)),
            out_shape=jax.ShapeDtypeStruct((tokens, chans), bf16),
            cost_estimate=cost(4 * size * halo_rows * chans, 4 << 20),
            name="finish",
        )(*halo_m, *back_m, *tap_f, *own_f, conv_bias, *pieces)
        every_channel = lax.all_gather(conv, "tp", axis=1, tiled=True)
        mixed = channel_mix(every_channel, channel_gain[layer], channel_shift[layer])
        update = jnp.dot(mixed, out_weight[layer], preferred_element_type=jnp.float32)
        state = (state.astype(jnp.float32) + update).astype(jnp.bfloat16)
    return state


def solution(mesh):
    return jax.shard_map(
        per_device,
        mesh=mesh,
        in_specs=(
            P("sp", None),
            P(),
            P(None, None, "tp"),
            P(None, None, "tp"),
            P(None, None, "tp"),
            P(None, "tp"),
            P(),
            P(),
            P(),
        ),
        out_specs=P("sp", None),
        check_vma=False,
    )
```

```python
import functools

import jax
import jax.numpy as jnp
import numpy as np
from jax import lax
from jax.experimental import pallas as pl
from jax.experimental.pallas import tpu as pltpu
from jax.sharding import PartitionSpec as P

STEP = 32
LIMIT = 20 << 20


def passed_along(value, axis, by):
    count = lax.axis_size(axis)
    pairs = [(i, (i + by) % count) for i in range(count) if by > 1 or i + by < count]
    return lax.ppermute(value, axis, pairs)


def scaled_rows(values, gain):
    scale = lax.rsqrt(jnp.mean(values * values, axis=-1, keepdims=True) + 1e-06)
    return (values * scale * gain).astype(jnp.bfloat16)


def gated_rows(normed, w_value, w_gate):
    values = dot(normed, w_value[...])
    gates = dot(normed, w_gate[...])
    return (values * jax.nn.sigmoid(gates)).astype(jnp.bfloat16)


def halves(rows):
    part = rows // 2 if rows % 32 == 0 else rows
    return [pl.ds(r, part) for r in range(0, rows, part)]


def first_gate_kernel(stream, gain, w_value, w_gate, gated, state, v_buf, g_buf, sems):
    pieces = halves(state.shape[0])
    copies = [pltpu.make_async_copy(stream.at[pieces[0]], state.at[pieces[0]], sems.at[0])]
    copies.append(pltpu.make_async_copy(w_value.at[0], v_buf, sems.at[1]))
    copies.append(pltpu.make_async_copy(w_gate.at[0], g_buf, sems.at[2]))
    for i, rows in enumerate(pieces[1:]):
        copies.append(pltpu.make_async_copy(stream.at[rows], state.at[rows], sems.at[3 + i]))
    for copy in copies:
        copy.start()
    copies[0].wait()
    normed = [scaled_rows(state[pieces[0], :].astype(jnp.float32), gain[0:1, :])]
    for copy in copies[1:]:
        copy.wait()
    for rows in pieces[1:]:
        normed.append(scaled_rows(state[rows, :].astype(jnp.float32), gain[0:1, :]))
    for rows, value in zip(pieces, normed):
        gated[rows, :] = gated_rows(value, v_buf, g_buf)


def mixed_rows(first, other, rows, here, gain, shift):
    own = first[rows, :].astype(jnp.float32)
    far = other[rows, :].astype(jnp.float32)
    values = jnp.concatenate([jnp.where(here == 0, own, far), jnp.where(here == 0, far, own)], axis=1)
    center = jnp.mean(values, axis=-1, keepdims=True)
    values = values - center
    spread = jnp.mean(jnp.square(values), axis=-1, keepdims=True)
    normed = values * lax.rsqrt(spread + 1e-05) * gain + shift
    return (normed * jax.nn.sigmoid(normed)).astype(jnp.bfloat16)


def mix_gate_kernel(
    here, own, far, ch_gain, ch_shift, w_out, state_h, gain, w_value, w_gate, new_state, gated, o_buf, v_buf, g_buf, state, sems, *, layer
):
    copies = [
        pltpu.make_async_copy(w_out.at[layer], o_buf, sems.at[0]),
        pltpu.make_async_copy(w_value.at[layer + 1], v_buf, sems.at[1]),
        pltpu.make_async_copy(w_gate.at[layer + 1], g_buf, sems.at[2]),
        pltpu.make_async_copy(state_h, state, sems.at[3]),
    ]
    for copy in copies:
        copy.start()
    pieces = halves(state.shape[0])
    at = slice(layer, layer + 1)
    mixed = [mixed_rows(own, far, rows, here[0], ch_gain[at, :], ch_shift[at, :]) for rows in pieces]
    copies[0].wait()
    copies[3].wait()
    for rows, value in zip(pieces, mixed):
        new_state[rows, :] = (state[rows, :].astype(jnp.float32) + dot(value, o_buf[...])).astype(jnp.bfloat16)
    copies[1].wait()
    copies[2].wait()
    for rows in pieces:
        normed = scaled_rows(new_state[rows, :].astype(jnp.float32), gain[layer + 1 : layer + 2, :])
        gated[rows, :] = gated_rows(normed, v_buf, g_buf)


def mix_kernel(here, own, far, ch_gain, ch_shift, w_out, state, out, o_buf, sems, *, layer):
    copy = pltpu.make_async_copy(w_out.at[layer], o_buf, sems.at[0])
    at = slice(layer, layer + 1)

    @pl.when(pl.program_id(0) == 0)
    def _():
        copy.start()

    rows = pl.ds(0, own.shape[0])
    mixed = mixed_rows(own, far, rows, here[0], ch_gain[at, :], ch_shift[at, :])

    @pl.when(pl.program_id(0) == 0)
    def _():
        copy.wait()

    out[...] = (state[...].astype(jnp.float32) + dot(mixed, o_buf[...])).astype(jnp.bfloat16)


def rotations(rows, cols, row_at, col_at, unit, scale):
    col = col_at(np.arange(cols, dtype=np.float64))
    coarse = row_at(np.arange(0, rows, STEP, dtype=np.float64))
    fine = row_at(np.arange(STEP, dtype=np.float64)) - row_at(np.float64(0))
    a = unit * np.outer(coarse, col)
    b = unit * np.outer(fine, col)
    both = [scale * np.cos(a), scale * np.sin(a), np.cos(b), np.sin(b)]
    return [x.astype(np.float32) for x in both]


def split(value, ref, rows, cols, apart):
    hi = value.astype(jnp.bfloat16)
    ref[rows, pl.ds(cols, value.shape[1])] = hi
    ref[rows, pl.ds(cols + apart, value.shape[1])] = (value - hi.astype(jnp.float32)).astype(jnp.bfloat16)


def dot(a, b):
    return jnp.dot(a, b, preferred_element_type=jnp.float32)


def parts(value):
    hi = value.astype(jnp.bfloat16)
    return hi, (value - hi.astype(jnp.float32)).astype(jnp.bfloat16)


def spread_rows(tables, i):
    ca, sa, cb, sb = tables
    c1 = ca[i : i + 1, :]
    s1 = sa[i : i + 1, :]
    c2 = cb[...]
    s2 = sb[...]
    return c1 * c2 - s1 * s2, s1 * c2 + c1 * s2


def forward_matrix(tables, out):
    half, span = out.shape[0] // 2, out.shape[1] // 2
    for i in range(tables[0].shape[0]):
        c, s = spread_rows(tables, i)
        split(c, out, pl.ds(i * STEP, STEP), 0, span)
        split(s, out, pl.ds(half + i * STEP, STEP), 0, span)


def prep_kernel(*refs):
    own_t, halo_t, back_t = refs[0:4], refs[4:8], refs[8:12]
    taps, own, halo, back, spectra = refs[12:17]
    forward_matrix(halo_t, halo)
    for layer in range(taps.shape[0]):
        t = taps[layer]
        spectra[layer] = dot(halo[...], jnp.concatenate([t, t], axis=0))
    forward_matrix(own_t, own)
    half = back.shape[1] // 4
    for i in range(back_t[0].shape[0]):
        c, s = spread_rows(back_t, i)
        rows = pl.ds(i * STEP, STEP)
        split(c, back, rows, 0, 2 * half)
        split(s, back, rows, half, 2 * half)


def own_kernel(matrix, gated, out):
    g = gated[...]
    missing = matrix.shape[1] // 2 - g.shape[0]
    if missing:
        g = jnp.concatenate([g, jnp.zeros((missing, g.shape[1]), g.dtype)], axis=0)
    out[...] = dot(matrix[...], jnp.concatenate([g, g], axis=0))


def finish_kernel(*refs, layer, pieces):
    halo, spectra, own, back, bias = refs[0:5]
    got = refs[5 : 5 + pieces]
    place, out = refs[5 + pieces : 7 + pieces]
    steps = range(pieces, 0, -1)
    window = [g[...] if n == 1 else jnp.where(place[0] < n, 0, g[...]).astype(jnp.bfloat16) for n, g in zip(steps, got)]
    far = dot(halo[...], jnp.concatenate(window * 2, axis=0))
    half = halo.shape[0] // 2
    w_c = own[:half, :] + far[:half]
    w_s = own[half:, :] + far[half:]
    h_c = spectra[layer, :half, :]
    h_s = spectra[layer, half:, :]
    re_hi, re_lo = parts(w_c * h_c + w_s * h_s)
    im_hi, im_lo = parts(w_s * h_c - w_c * h_s)
    y = dot(back[...], jnp.concatenate([re_hi, im_hi, re_hi, im_hi], axis=0))
    y += dot(back[:, : 2 * half], jnp.concatenate([re_lo, im_lo], axis=0))
    out[...] = (y + bias[layer : layer + 1, :]).astype(jnp.bfloat16)


def cost(flops, size):
    return pl.CostEstimate(flops=flops, bytes_accessed=size, transcendentals=0)


def per_device(
    stream,
    norm_gain,
    value_weight,
    gate_weight,
    conv_taps,
    conv_bias,
    channel_gain,
    channel_shift,
    out_weight,
):
    tokens = stream.shape[0]
    layers, width, chans = conv_taps.shape
    halo_rows = -(-(width - 1) // 128) * 128
    hops = -(-halo_rows // tokens)
    size = -(-(tokens + halo_rows) // 512) * 512
    half = size // 2
    unit = 2 * np.pi / size
    bf16, f32 = jnp.bfloat16, jnp.float32
    assert tokens % STEP == 0 and halo_rows >= width

    def freq(k):
        return k + 0.5

    span = -(-tokens // 128) * 128
    own_tab = rotations(half, span, freq, lambda t: t + 1, unit, 1.0)
    halo_tab = rotations(half, halo_rows, freq, lambda i: i + 1 - halo_rows, unit, 1.0)
    back_tab = rotations(tokens, half, lambda t: t + 1, freq, unit, 2.0 / size)
    taps = conv_taps
    if halo_rows > width:
        taps = jnp.pad(conv_taps, ((0, 0), (halo_rows - width, 0), (0, 0)))

    here = lax.axis_index("tp").astype(jnp.int32)[None]
    place = lax.axis_index("sp").astype(jnp.int32)[None]
    width_in = stream.shape[1]
    vmem, hbm, smem = (pl.BlockSpec(memory_space=m) for m in (pltpu.VMEM, pltpu.HBM, pltpu.SMEM))
    buf = pltpu.VMEM((width_in, chans), bf16)
    out_buf = pltpu.VMEM(out_weight.shape[1:], bf16)

    def held(*arrays):
        return [pltpu.with_memory_space_constraint(a, pltpu.VMEM) for a in arrays]

    def remote(*arrays):
        return [pltpu.with_memory_space_constraint(a, pltpu.HBM) for a in arrays]

    own_m, halo_m, back_m, spectra = pl.pallas_call(
        prep_kernel,
        out_shape=[
            jax.ShapeDtypeStruct((size, 2 * span), bf16),
            jax.ShapeDtypeStruct((size, 2 * halo_rows), bf16),
            jax.ShapeDtypeStruct((tokens, 2 * size), bf16),
            jax.ShapeDtypeStruct((layers, size, chans), f32),
        ],
        cost_estimate=cost(8 * layers * size * halo_rows * chans, 8 << 20),
        compiler_params=pltpu.CompilerParams(vmem_limit_bytes=LIMIT),
        name="prep",
    )(*own_tab, *halo_tab, *back_tab, taps)

    rows_buf = pltpu.VMEM((tokens, width_in), bf16)
    own_gated = pl.pallas_call(
        first_gate_kernel,
        in_specs=[hbm, vmem, hbm, hbm],
        out_shape=pltpu.VMEM((tokens, chans), bf16),
        out_specs=vmem,
        scratch_shapes=[rows_buf, buf, buf, pltpu.SemaphoreType.DMA((4,))],
        compiler_params=pltpu.CompilerParams(vmem_limit_bytes=LIMIT),
        name="first_gate",
    )(*remote(stream), norm_gain, *remote(value_weight, gate_weight))
    state = stream
    for layer in range(layers):
        pieces = []
        for step in range(1, hops + 1):
            count = min(tokens, halo_rows - (step - 1) * tokens)
            pieces.insert(0, passed_along(own_gated[tokens - count :], "sp", step))
        own_f = pl.pallas_call(
            own_kernel,
            in_specs=[vmem] * 2,
            out_shape=jax.ShapeDtypeStruct((size, chans), f32),
            cost_estimate=cost(8 * size * tokens * chans, 4 << 20),
            compiler_params=pltpu.CompilerParams(vmem_limit_bytes=LIMIT),
            name="own_part",
        )(own_m, own_gated)
        conv = pl.pallas_call(
            functools.partial(finish_kernel, layer=layer, pieces=len(pieces)),
            in_specs=[vmem] * (5 + len(pieces)) + [smem],
            out_shape=pltpu.VMEM((tokens, chans), bf16),
            out_specs=vmem,
            cost_estimate=cost(8 * size * halo_rows * chans, 4 << 20),
            compiler_params=pltpu.CompilerParams(vmem_limit_bytes=LIMIT),
            name="finish",
        )(halo_m, spectra, own_f, back_m, conv_bias, *pieces, place)
        far = lax.ppermute(conv, "tp", [(0, 1), (1, 0)])
        if layer + 1 < layers:
            state, own_gated = pl.pallas_call(
                functools.partial(mix_gate_kernel, layer=layer),
                in_specs=[smem, vmem, vmem, vmem, vmem, hbm, hbm, vmem, hbm, hbm],
                out_shape=[pltpu.VMEM((tokens, width_in), bf16), pltpu.VMEM((tokens, chans), bf16)],
                out_specs=[vmem, vmem],
                scratch_shapes=[out_buf, buf, buf, rows_buf, pltpu.SemaphoreType.DMA((4,))],
                compiler_params=pltpu.CompilerParams(vmem_limit_bytes=LIMIT),
                name="mix_gate",
            )(
                here,
                *held(conv, far),
                channel_gain,
                channel_shift,
                *remote(out_weight, state),
                norm_gain,
                *remote(value_weight, gate_weight),
            )
    steps = 4 if tokens % 64 == 0 else 1
    rows = tokens // steps

    def block(cols):
        return pl.BlockSpec((rows, cols), lambda i: (i, 0))

    def whole(array):
        return pl.BlockSpec(array.shape, lambda i: (0, 0))

    return pl.pallas_call(
        functools.partial(mix_kernel, layer=layers - 1),
        grid=(steps,),
        in_specs=[smem, block(chans), block(chans), whole(channel_gain), whole(channel_shift), hbm, block(width_in)],
        out_shape=jax.ShapeDtypeStruct((tokens, width_in), bf16),
        out_specs=block(width_in),
        scratch_shapes=[out_buf, pltpu.SemaphoreType.DMA((1,))],
        compiler_params=pltpu.CompilerParams(vmem_limit_bytes=LIMIT),
        name="mix",
    )(here, conv, far, channel_gain, channel_shift, *remote(out_weight), state)


def solution(mesh):
    return jax.shard_map(
        per_device,
        mesh=mesh,
        in_specs=(
            P("sp", None),
            P(),
            P(None, None, "tp"),
            P(None, None, "tp"),
            P(None, None, "tp"),
            P(None, "tp"),
            P(),
            P(),
            P(),
        ),
        out_specs=P("sp", None),
        check_vma=False,
    )
```

```python
import functools

import jax
import jax.numpy as jnp
import numpy as np
from jax import lax
from jax.experimental import pallas as pl
from jax.experimental.pallas import tpu as pltpu
from jax.sharding import PartitionSpec as P

STEP = 32
LIMIT = 20 << 20


def passed_along(value, axis, by):
    count = lax.axis_size(axis)
    pairs = [(i, (i + by) % count) for i in range(count) if by > 1 or i + by < count]
    return lax.ppermute(value, axis, pairs)


def chunks(total, part):
    part = part if total % part == 0 else total
    return [pl.ds(r, part) for r in range(0, total, part)]


def gate_all(normed, w_value, w_gate, gated, tail):
    values = dot(normed[...], w_value[...])
    gates = dot(normed[...], w_gate[...])
    out = (values * jax.nn.sigmoid(gates)).astype(jnp.bfloat16)
    gated[...] = out
    tail[...] = out[out.shape[0] - tail.shape[0] :]


def first_gate_kernel(stream, gain_h, w_value, w_gate, tail, gated, state, normed, gain, v_buf, g_buf, sems):
    total = state.shape[0]
    pieces = chunks(total, 64)
    copies = [pltpu.make_async_copy(gain_h, gain, sems.at[0])]
    for i, rows in enumerate(pieces):
        copies.append(pltpu.make_async_copy(stream.at[rows], state.at[rows], sems.at[3 + i]))
    copies.append(pltpu.make_async_copy(w_value.at[0], v_buf, sems.at[1]))
    copies.append(pltpu.make_async_copy(w_gate.at[0], g_buf, sems.at[2]))
    for copy in copies:
        copy.start()
    copies[0].wait()
    for i, piece in enumerate(pieces):
        copies[1 + i].wait()
        for part in chunks(piece.size, 32):
            rows = pl.ds(piece.start + part.start, part.size)
            values = state[rows, :].astype(jnp.float32)
            scale = lax.rsqrt(jnp.mean(values * values, axis=-1, keepdims=True) + 1e-06)
            normed[rows, :] = (values * scale * gain[0:1, :]).astype(jnp.bfloat16)
    copies[-2].wait()
    copies[-1].wait()
    gate_all(normed, v_buf, g_buf, gated, tail)


def mix_all(first, other, gain, shift, mixed):
    here = lax.axis_index("tp")
    for rows in chunks(mixed.shape[0], 64):
        own = first[rows, :].astype(jnp.float32)
        far = other[rows, :].astype(jnp.float32)
        values = jnp.concatenate([jnp.where(here == 0, own, far), jnp.where(here == 0, far, own)], axis=1)
        center = jnp.mean(values, axis=-1, keepdims=True)
        values = values - center
        spread = jnp.mean(jnp.square(values), axis=-1, keepdims=True)
        normed = values * lax.rsqrt(spread + 1e-05) * gain + shift
        mixed[rows, :] = (normed * jax.nn.sigmoid(normed)).astype(jnp.bfloat16)


def mix_gate_kernel(
    own, far, ch_gain, ch_shift, w_out, state, gain, w_value, w_gate,
    new_state, gated, tail, mixed, normed, v_buf, g_buf, sems, *, layer
):
    copies = [
        pltpu.make_async_copy(w_value.at[layer + 1], v_buf, sems.at[0]),
        pltpu.make_async_copy(w_gate.at[layer + 1], g_buf, sems.at[1]),
    ]
    for copy in copies:
        copy.start()
    at = slice(layer, layer + 1)
    mix_all(own, far, ch_gain[at, :], ch_shift[at, :], mixed)
    width = new_state.shape[1]
    total = 0.0
    for cols in chunks(width, 512):
        update = dot(mixed[...], w_out[layer, :, cols])
        new = (state[:, cols].astype(jnp.float32) + update).astype(jnp.bfloat16)
        new_state[:, cols] = new
        new = new.astype(jnp.float32)
        total += jnp.sum(new * new, axis=-1, keepdims=True)
    scale = lax.rsqrt(total / width + 1e-06)
    for cols in chunks(width, 512):
        values = new_state[:, cols].astype(jnp.float32)
        normed[:, cols] = (values * scale * gain[layer + 1 : layer + 2, cols]).astype(jnp.bfloat16)
    for copy in copies:
        copy.wait()
    gate_all(normed, v_buf, g_buf, gated, tail)


def mix_kernel(own, far, ch_gain, ch_shift, w_out, state, out_h, mixed, out, sems, *, layer):
    at = slice(layer, layer + 1)
    mix_all(own, far, ch_gain[at, :], ch_shift[at, :], mixed)
    copies = []
    for i, cols in enumerate(chunks(state.shape[1], 512)):
        update = dot(mixed[...], w_out[layer, :, cols])
        out[:, cols] = (state[:, cols].astype(jnp.float32) + update).astype(jnp.bfloat16)
        copies.append(pltpu.make_async_copy(out.at[:, cols], out_h.at[:, cols], sems.at[i]))
        copies[-1].start()
    for copy in copies:
        copy.wait()


def rotations(rows, cols, row_at, col_at, unit, scale):
    col = col_at(np.arange(cols, dtype=np.float64))
    coarse = row_at(np.arange(0, rows, STEP, dtype=np.float64))
    fine = row_at(np.arange(STEP, dtype=np.float64)) - row_at(np.float64(0))
    a = unit * np.outer(coarse, col)
    b = unit * np.outer(fine, col)
    both = [scale * np.cos(a), scale * np.sin(a), np.cos(b), np.sin(b)]
    return [x.astype(np.float32) for x in both]


def split(value, ref, rows, cols, apart):
    hi = value.astype(jnp.bfloat16)
    ref[rows, pl.ds(cols, value.shape[1])] = hi
    ref[rows, pl.ds(cols + apart, value.shape[1])] = (value - hi.astype(jnp.float32)).astype(jnp.bfloat16)


def dot(a, b):
    return jnp.dot(a, b, preferred_element_type=jnp.float32)


def parts(value):
    hi = value.astype(jnp.bfloat16)
    return hi, (value - hi.astype(jnp.float32)).astype(jnp.bfloat16)


def spread_rows(tables, i):
    ca, sa, cb, sb = tables
    c1 = ca[i : i + 1, :]
    s1 = sa[i : i + 1, :]
    c2 = cb[...]
    s2 = sb[...]
    return c1 * c2 - s1 * s2, s1 * c2 + c1 * s2


def forward_matrix(tables, out):
    half, span = out.shape[0] // 2, out.shape[1] // 2
    for i in range(tables[0].shape[0]):
        c, s = spread_rows(tables, i)
        split(c, out, pl.ds(i * STEP, STEP), 0, span)
        split(s, out, pl.ds(half + i * STEP, STEP), 0, span)


def prep_kernel(*refs):
    own_t, halo_t, back_t = refs[0:4], refs[4:8], refs[8:12]
    taps, own, halo, back, spectra = refs[12:17]
    forward_matrix(halo_t, halo)
    for layer in range(taps.shape[0]):
        t = taps[layer]
        spectra[layer] = dot(halo[...], jnp.concatenate([t, t], axis=0))
    forward_matrix(own_t, own)
    half = back.shape[1] // 4
    for i in range(back_t[0].shape[0]):
        c, s = spread_rows(back_t, i)
        rows = pl.ds(i * STEP, STEP)
        split(c, back, rows, 0, 2 * half)
        split(s, back, rows, half, 2 * half)


def own_kernel(matrix, gated, out):
    g = gated[...]
    missing = matrix.shape[1] // 2 - g.shape[0]
    if missing:
        g = jnp.concatenate([g, jnp.zeros((missing, g.shape[1]), g.dtype)], axis=0)
    out[...] = dot(matrix[...], jnp.concatenate([g, g], axis=0))


def finish_kernel(*refs, layer, pieces):
    halo, spectra, own, back, bias = refs[0:5]
    got = refs[5 : 5 + pieces]
    out = refs[5 + pieces]
    place = lax.axis_index("sp")
    steps = range(pieces, 0, -1)
    window = [g[...] if n == 1 else jnp.where(place < n, 0, g[...]).astype(jnp.bfloat16) for n, g in zip(steps, got)]
    far = dot(halo[...], jnp.concatenate(window * 2, axis=0))
    half = halo.shape[0] // 2
    w_c = own[:half, :] + far[:half]
    w_s = own[half:, :] + far[half:]
    h_c = spectra[layer, :half, :]
    h_s = spectra[layer, half:, :]
    re_hi, re_lo = parts(w_c * h_c + w_s * h_s)
    im_hi, im_lo = parts(w_s * h_c - w_c * h_s)
    y = dot(back[...], jnp.concatenate([re_hi, im_hi, re_hi, im_hi], axis=0))
    y += dot(back[:, : 2 * half], jnp.concatenate([re_lo, im_lo], axis=0))
    out[...] = (y + bias[layer : layer + 1, :]).astype(jnp.bfloat16)


def cost(flops, size):
    return pl.CostEstimate(flops=flops, bytes_accessed=size, transcendentals=0)


def per_device(
    stream,
    norm_gain,
    value_weight,
    gate_weight,
    conv_taps,
    conv_bias,
    channel_gain,
    channel_shift,
    out_weight,
):
    tokens = stream.shape[0]
    layers, width, chans = conv_taps.shape
    halo_rows = -(-(width - 1) // 128) * 128
    hops = -(-halo_rows // tokens)
    size = -(-(tokens + halo_rows) // 512) * 512
    half = size // 2
    unit = 2 * np.pi / size
    bf16, f32 = jnp.bfloat16, jnp.float32
    assert tokens % STEP == 0 and halo_rows >= width

    def freq(k):
        return k + 0.5

    span = -(-tokens // 128) * 128
    own_tab = rotations(half, span, freq, lambda t: t + 1, unit, 1.0)
    halo_tab = rotations(half, halo_rows, freq, lambda i: i + 1 - halo_rows, unit, 1.0)
    back_tab = rotations(tokens, half, lambda t: t + 1, freq, unit, 2.0 / size)
    taps = conv_taps
    if halo_rows > width:
        taps = jnp.pad(conv_taps, ((0, 0), (halo_rows - width, 0), (0, 0)))

    width_in = stream.shape[1]
    vmem, hbm = (pl.BlockSpec(memory_space=m) for m in (pltpu.VMEM, pltpu.HBM))
    buf = pltpu.VMEM((width_in, chans), bf16)
    last = halo_rows - (hops - 1) * tokens
    columns = len(chunks(width_in, 512))
    params = pltpu.CompilerParams(vmem_limit_bytes=LIMIT)

    def remote(*arrays):
        return [pltpu.with_memory_space_constraint(a, pltpu.HBM) for a in arrays]

    own_m, halo_m, back_m, spectra = pl.pallas_call(
        prep_kernel,
        out_shape=[
            jax.ShapeDtypeStruct((size, 2 * span), bf16),
            jax.ShapeDtypeStruct((size, 2 * halo_rows), bf16),
            jax.ShapeDtypeStruct((tokens, 2 * size), bf16),
            jax.ShapeDtypeStruct((layers, size, chans), f32),
        ],
        cost_estimate=cost(8 * layers * size * halo_rows * chans, 8 << 20),
        compiler_params=pltpu.CompilerParams(vmem_limit_bytes=LIMIT),
        name="prep",
    )(*own_tab, *halo_tab, *back_tab, taps)

    rows_buf = pltpu.VMEM((tokens, width_in), bf16)
    mixed_buf = pltpu.VMEM((tokens, out_weight.shape[1]), bf16)
    gated_out = [pltpu.VMEM((tokens, chans), bf16), pltpu.VMEM((last, chans), bf16)]
    tail, own_gated = pl.pallas_call(
        first_gate_kernel,
        in_specs=[hbm] * 4,
        out_shape=gated_out[::-1],
        out_specs=[vmem] * 2,
        scratch_shapes=[
            rows_buf,
            rows_buf,
            pltpu.VMEM(norm_gain.shape, f32),
            buf,
            buf,
            pltpu.SemaphoreType.DMA((3 + len(chunks(tokens, 64)),)),
        ],
        compiler_params=params,
        name="first_gate",
    )(*remote(stream, norm_gain, value_weight, gate_weight))
    state = stream
    for layer in range(layers):
        pieces = []
        for step in range(hops, 0, -1):
            pieces.append(passed_along(own_gated if step < hops else tail, "sp", step))
        own_f = pl.pallas_call(
            own_kernel,
            in_specs=[vmem] * 2,
            out_shape=jax.ShapeDtypeStruct((size, chans), f32),
            cost_estimate=cost(8 * size * tokens * chans, 4 << 20),
            compiler_params=params,
            name="own_part",
        )(own_m, own_gated)
        conv = pl.pallas_call(
            functools.partial(finish_kernel, layer=layer, pieces=len(pieces)),
            in_specs=[vmem] * (5 + len(pieces)),
            out_shape=pltpu.VMEM((tokens, chans), bf16),
            out_specs=vmem,
            cost_estimate=cost(8 * size * halo_rows * chans, 4 << 20),
            compiler_params=params,
            name="finish",
        )(halo_m, spectra, own_f, back_m, conv_bias, *pieces)
        far = lax.ppermute(conv, "tp", [(0, 1), (1, 0)])
        if layer + 1 < layers:
            state, own_gated, tail = pl.pallas_call(
                functools.partial(mix_gate_kernel, layer=layer),
                in_specs=[vmem] * 7 + [hbm] * 2,
                out_shape=[pltpu.VMEM((tokens, width_in), bf16)] + gated_out,
                out_specs=[vmem] * 3,
                scratch_shapes=[mixed_buf, rows_buf, buf, buf, pltpu.SemaphoreType.DMA((2,))],
                compiler_params=params,
                name="mix_gate",
            )(conv, far, channel_gain, channel_shift, out_weight, state, norm_gain, *remote(value_weight, gate_weight))
    return pl.pallas_call(
        functools.partial(mix_kernel, layer=layers - 1),
        in_specs=[vmem] * 6,
        out_shape=jax.ShapeDtypeStruct((tokens, width_in), bf16),
        out_specs=hbm,
        scratch_shapes=[mixed_buf, rows_buf, pltpu.SemaphoreType.DMA((columns,))],
        compiler_params=params,
        name="mix",
    )(conv, far, channel_gain, channel_shift, out_weight, state)


def solution(mesh):
    return jax.shard_map(
        per_device,
        mesh=mesh,
        in_specs=(
            P("sp", None),
            P(),
            P(None, None, "tp"),
            P(None, None, "tp"),
            P(None, None, "tp"),
            P(None, "tp"),
            P(),
            P(),
            P(),
        ),
        out_specs=P("sp", None),
        check_vma=False,
    )
```

```python
import functools

import jax
import jax.numpy as jnp
import numpy as np
from jax import lax
from jax.experimental import pallas as pl
from jax.experimental.pallas import tpu as pltpu
from jax.sharding import PartitionSpec as P

STEP = 32
LIMIT = 20 << 20


def passed_along(value, axis, by):
    count = lax.axis_size(axis)
    pairs = [(i, (i + by) % count) for i in range(count) if by > 1 or i + by < count]
    return lax.ppermute(value, axis, pairs)


def chunks(total, part):
    part = part if total % part == 0 else total
    return [pl.ds(r, part) for r in range(0, total, part)]


def gate_all(normed, w_value, w_gate, gated, tail):
    values = dot(normed[...], w_value[...])
    gates = dot(normed[...], w_gate[...])
    out = (values * jax.nn.sigmoid(gates)).astype(jnp.bfloat16)
    gated[...] = out
    if tail is not None:
        tail[...] = out[out.shape[0] - tail.shape[0] :]


def first_gate_kernel(stream, gain_h, w_value, w_gate, gated, state, normed, gain, v_buf, g_buf, sems):
    total = state.shape[0]
    pieces = chunks(total, 64)
    copies = [pltpu.make_async_copy(gain_h, gain, sems.at[0])]
    for i, rows in enumerate(pieces):
        copies.append(pltpu.make_async_copy(stream.at[rows], state.at[rows], sems.at[3 + i]))
    copies.append(pltpu.make_async_copy(w_value.at[0], v_buf, sems.at[1]))
    copies.append(pltpu.make_async_copy(w_gate.at[0], g_buf, sems.at[2]))
    for copy in copies:
        copy.start()
    copies[0].wait()
    for i, piece in enumerate(pieces):
        copies[1 + i].wait()
        for part in chunks(piece.size, 32):
            rows = pl.ds(piece.start + part.start, part.size)
            values = state[rows, :].astype(jnp.float32)
            scale = lax.rsqrt(jnp.mean(values * values, axis=-1, keepdims=True) + 1e-06)
            normed[rows, :] = (values * scale * gain[0:1, :]).astype(jnp.bfloat16)
    copies[-2].wait()
    copies[-1].wait()
    gate_all(normed, v_buf, g_buf, gated, None)


def mix_all(first, other, gain, shift, mixed):
    here = lax.axis_index("tp")
    for rows in chunks(mixed.shape[0], 64):
        own = first[rows, :].astype(jnp.float32)
        far = other[rows, :].astype(jnp.float32)
        values = jnp.concatenate([jnp.where(here == 0, own, far), jnp.where(here == 0, far, own)], axis=1)
        center = jnp.mean(values, axis=-1, keepdims=True)
        values = values - center
        spread = jnp.mean(jnp.square(values), axis=-1, keepdims=True)
        normed = values * lax.rsqrt(spread + 1e-05) * gain + shift
        mixed[rows, :] = (normed * jax.nn.sigmoid(normed)).astype(jnp.bfloat16)


def mix_gate_kernel(
    own, far, ch_gain, ch_shift, w_out, state, gain, w_value, w_gate,
    new_state, gated, tail, mixed, normed, v_buf, g_buf, sems, *, layer
):
    copies = [
        pltpu.make_async_copy(w_value.at[layer + 1], v_buf, sems.at[0]),
        pltpu.make_async_copy(w_gate.at[layer + 1], g_buf, sems.at[1]),
    ]
    for copy in copies:
        copy.start()
    at = slice(layer, layer + 1)
    mix_all(own, far, ch_gain[at, :], ch_shift[at, :], mixed)
    width = new_state.shape[1]
    total = 0.0
    for cols in chunks(width, 512):
        update = dot(mixed[...], w_out[layer, :, cols])
        new = (state[:, cols].astype(jnp.float32) + update).astype(jnp.bfloat16)
        new_state[:, cols] = new
        new = new.astype(jnp.float32)
        total += jnp.sum(new * new, axis=-1, keepdims=True)
    scale = lax.rsqrt(total / width + 1e-06)
    for cols in chunks(width, 512):
        values = new_state[:, cols].astype(jnp.float32)
        normed[:, cols] = (values * scale * gain[layer + 1 : layer + 2, cols]).astype(jnp.bfloat16)
    for copy in copies:
        copy.wait()
    gate_all(normed, v_buf, g_buf, gated, tail)


def mix_kernel(own, far, ch_gain, ch_shift, w_out, state, out_h, mixed, out, sems, *, layer):
    at = slice(layer, layer + 1)
    mix_all(own, far, ch_gain[at, :], ch_shift[at, :], mixed)
    copies = []
    for i, cols in enumerate(chunks(state.shape[1], 512)):
        update = dot(mixed[...], w_out[layer, :, cols])
        out[:, cols] = (state[:, cols].astype(jnp.float32) + update).astype(jnp.bfloat16)
        copies.append(pltpu.make_async_copy(out.at[:, cols], out_h.at[:, cols], sems.at[i]))
        copies[-1].start()
    for copy in copies:
        copy.wait()


def rotations(rows, cols, row_at, col_at, unit, scale):
    col = col_at(np.arange(cols, dtype=np.float64))
    coarse = row_at(np.arange(0, rows, STEP, dtype=np.float64))
    fine = row_at(np.arange(STEP, dtype=np.float64)) - row_at(np.float64(0))
    a = unit * np.outer(coarse, col)
    b = unit * np.outer(fine, col)
    both = [scale * np.cos(a), scale * np.sin(a), np.cos(b), np.sin(b)]
    return [x.astype(np.float32) for x in both]


def split(value, ref, rows, cols, apart):
    hi = value.astype(jnp.bfloat16)
    ref[rows, pl.ds(cols, value.shape[1])] = hi
    ref[rows, pl.ds(cols + apart, value.shape[1])] = (value - hi.astype(jnp.float32)).astype(jnp.bfloat16)


def dot(a, b):
    return jnp.dot(a, b, preferred_element_type=jnp.float32)


def parts(value):
    hi = value.astype(jnp.bfloat16)
    return hi, (value - hi.astype(jnp.float32)).astype(jnp.bfloat16)


def spread_rows(tables, i):
    ca, sa, cb, sb = tables
    c1 = ca[i : i + 1, :]
    s1 = sa[i : i + 1, :]
    c2 = cb[...]
    s2 = sb[...]
    return c1 * c2 - s1 * s2, s1 * c2 + c1 * s2


def forward_matrix(tables, out):
    half, span = out.shape[0] // 2, out.shape[1] // 2
    for i in range(tables[0].shape[0]):
        c, s = spread_rows(tables, i)
        split(c, out, pl.ds(i * STEP, STEP), 0, span)
        split(s, out, pl.ds(half + i * STEP, STEP), 0, span)


def prep_kernel(*refs):
    own_t, halo_t, back_t = refs[0:4], refs[4:8], refs[8:12]
    taps, gated, own, halo, back, spectra, tail = refs[12:19]
    tail[...] = gated[gated.shape[0] - tail.shape[0] :, :]
    forward_matrix(halo_t, halo)
    for layer in range(taps.shape[0]):
        t = taps[layer]
        spectra[layer] = dot(halo[...], jnp.concatenate([t, t], axis=0))
    forward_matrix(own_t, own)
    half = back.shape[1] // 4
    for i in range(back_t[0].shape[0]):
        c, s = spread_rows(back_t, i)
        rows = pl.ds(i * STEP, STEP)
        split(c, back, rows, 0, 2 * half)
        split(s, back, rows, half, 2 * half)


def own_kernel(matrix, gated, out):
    g = gated[...]
    missing = matrix.shape[1] // 2 - g.shape[0]
    if missing:
        g = jnp.concatenate([g, jnp.zeros((missing, g.shape[1]), g.dtype)], axis=0)
    out[...] = dot(matrix[...], jnp.concatenate([g, g], axis=0))


def finish_kernel(*refs, layer, pieces):
    halo, spectra, own, back, bias = refs[0:5]
    got = refs[5 : 5 + pieces]
    out = refs[5 + pieces]
    place = lax.axis_index("sp")
    steps = range(pieces, 0, -1)
    window = [g[...] if n == 1 else jnp.where(place < n, 0, g[...]).astype(jnp.bfloat16) for n, g in zip(steps, got)]
    far = dot(halo[...], jnp.concatenate(window * 2, axis=0))
    half = halo.shape[0] // 2
    w_c = own[:half, :] + far[:half]
    w_s = own[half:, :] + far[half:]
    h_c = spectra[layer, :half, :]
    h_s = spectra[layer, half:, :]
    re_hi, re_lo = parts(w_c * h_c + w_s * h_s)
    im_hi, im_lo = parts(w_s * h_c - w_c * h_s)
    y = dot(back[...], jnp.concatenate([re_hi, im_hi, re_hi, im_hi], axis=0))
    y += dot(back[:, : 2 * half], jnp.concatenate([re_lo, im_lo], axis=0))
    out[...] = (y + bias[layer : layer + 1, :]).astype(jnp.bfloat16)


def cost(flops, size):
    return pl.CostEstimate(flops=flops, bytes_accessed=size, transcendentals=0)


def per_device(
    stream,
    norm_gain,
    value_weight,
    gate_weight,
    conv_taps,
    conv_bias,
    channel_gain,
    channel_shift,
    out_weight,
):
    tokens = stream.shape[0]
    layers, width, chans = conv_taps.shape
    halo_rows = -(-(width - 1) // 128) * 128
    hops = -(-halo_rows // tokens)
    size = -(-(tokens + halo_rows) // 512) * 512
    half = size // 2
    unit = 2 * np.pi / size
    bf16, f32 = jnp.bfloat16, jnp.float32
    assert tokens % STEP == 0 and halo_rows >= width

    def freq(k):
        return k + 0.5

    span = -(-tokens // 128) * 128
    own_tab = rotations(half, span, freq, lambda t: t + 1, unit, 1.0)
    halo_tab = rotations(half, halo_rows, freq, lambda i: i + 1 - halo_rows, unit, 1.0)
    back_tab = rotations(tokens, half, lambda t: t + 1, freq, unit, 2.0 / size)
    taps = conv_taps
    if halo_rows > width:
        taps = jnp.pad(conv_taps, ((0, 0), (halo_rows - width, 0), (0, 0)))

    width_in = stream.shape[1]
    vmem, hbm = (pl.BlockSpec(memory_space=m) for m in (pltpu.VMEM, pltpu.HBM))
    buf = pltpu.VMEM((width_in, chans), bf16)
    last = halo_rows - (hops - 1) * tokens
    columns = len(chunks(width_in, 512))
    params = pltpu.CompilerParams(vmem_limit_bytes=LIMIT)

    def remote(*arrays):
        return [pltpu.with_memory_space_constraint(a, pltpu.HBM) for a in arrays]

    rows_buf = pltpu.VMEM((tokens, width_in), bf16)
    mixed_buf = pltpu.VMEM((tokens, out_weight.shape[1]), bf16)
    gated_out = [pltpu.VMEM((tokens, chans), bf16), pltpu.VMEM((last, chans), bf16)]
    own_gated = pl.pallas_call(
        first_gate_kernel,
        in_specs=[hbm] * 4,
        out_shape=gated_out[0],
        out_specs=vmem,
        scratch_shapes=[
            rows_buf,
            rows_buf,
            pltpu.VMEM(norm_gain.shape, f32),
            buf,
            buf,
            pltpu.SemaphoreType.DMA((3 + len(chunks(tokens, 64)),)),
        ],
        compiler_params=params,
        name="first_gate",
    )(*remote(stream, norm_gain, value_weight, gate_weight))
    own_m, halo_m, back_m, spectra, tail = pl.pallas_call(
        prep_kernel,
        out_shape=[
            jax.ShapeDtypeStruct((size, 2 * span), bf16),
            jax.ShapeDtypeStruct((size, 2 * halo_rows), bf16),
            jax.ShapeDtypeStruct((tokens, 2 * size), bf16),
            jax.ShapeDtypeStruct((layers, size, chans), f32),
            pltpu.VMEM((last, chans), bf16),
        ],
        cost_estimate=cost(8 * layers * size * halo_rows * chans, 8 << 20),
        compiler_params=pltpu.CompilerParams(vmem_limit_bytes=LIMIT),
        name="prep",
    )(*own_tab, *halo_tab, *back_tab, taps, own_gated)

    state = stream
    for layer in range(layers):
        pieces = []
        for step in range(hops, 0, -1):
            pieces.append(passed_along(own_gated if step < hops else tail, "sp", step))
        own_f = pl.pallas_call(
            own_kernel,
            in_specs=[vmem] * 2,
            out_shape=jax.ShapeDtypeStruct((size, chans), f32),
            cost_estimate=cost(8 * size * tokens * chans, 4 << 20),
            compiler_params=params,
            name="own_part",
        )(own_m, own_gated)
        conv = pl.pallas_call(
            functools.partial(finish_kernel, layer=layer, pieces=len(pieces)),
            in_specs=[vmem] * (5 + len(pieces)),
            out_shape=pltpu.VMEM((tokens, chans), bf16),
            out_specs=vmem,
            cost_estimate=cost(8 * size * halo_rows * chans, 4 << 20),
            compiler_params=params,
            name="finish",
        )(halo_m, spectra, own_f, back_m, conv_bias, *pieces)
        far = lax.ppermute(conv, "tp", [(0, 1), (1, 0)])
        if layer + 1 < layers:
            state, own_gated, tail = pl.pallas_call(
                functools.partial(mix_gate_kernel, layer=layer),
                in_specs=[vmem] * 7 + [hbm] * 2,
                out_shape=[pltpu.VMEM((tokens, width_in), bf16)] + gated_out,
                out_specs=[vmem] * 3,
                scratch_shapes=[mixed_buf, rows_buf, buf, buf, pltpu.SemaphoreType.DMA((2,))],
                compiler_params=params,
                name="mix_gate",
            )(conv, far, channel_gain, channel_shift, out_weight, state, norm_gain, *remote(value_weight, gate_weight))
    return pl.pallas_call(
        functools.partial(mix_kernel, layer=layers - 1),
        in_specs=[vmem] * 6,
        out_shape=jax.ShapeDtypeStruct((tokens, width_in), bf16),
        out_specs=hbm,
        scratch_shapes=[mixed_buf, rows_buf, pltpu.SemaphoreType.DMA((columns,))],
        compiler_params=params,
        name="mix",
    )(conv, far, channel_gain, channel_shift, out_weight, state)


def solution(mesh):
    return jax.shard_map(
        per_device,
        mesh=mesh,
        in_specs=(
            P("sp", None),
            P(),
            P(None, None, "tp"),
            P(None, None, "tp"),
            P(None, None, "tp"),
            P(None, "tp"),
            P(),
            P(),
            P(),
        ),
        out_specs=P("sp", None),
        check_vma=False,
    )
```
